32 devices in a mesh: kv: 8 (over z, y), tp: 4 (over x, core).
Axes of the slice: x: 2, y: 2, z: 4, core: 2. Of those that a mesh axis runs over, the one named last changes fastest.
Arguments:
- tokens: bfloat16 [16, 4096], P(None, ('kv', 'tp')), may hold values from -6 to 6
- gain_attn: bfloat16 [4096], replicated, may hold values from 0.099609375 to 1.8984375
- w_query: bfloat16 [4096, 2048], P('kv', 'tp'), may hold values from -0.09375 to 0.09375
- w_key: bfloat16 [4096, 2048], P('kv', 'tp'), may hold values from -0.09375 to 0.09375
- w_value: bfloat16 [4096, 2048], P('kv', 'tp'), may hold values from -0.09375 to 0.09375
- w_forget: bfloat16 [4096, 32], replicated, may hold values from -0.09375 to 0.09375
- forget_bias: float32 [32], replicated, may hold values from -2 to 2
- keys_cache: bfloat16 [16, 4096, 2048], P(None, 'kv', 'tp'), may hold values from -900 to 900
- values_cache: bfloat16 [16, 4096, 2048], P(None, 'kv', 'tp'), may hold values from -6 to 6
- gates_cache: float32 [16, 32, 4096], P(None, 'tp', 'kv'), as said below
- lengths: int32 [16], replicated, may hold values from 1 to 4096, 32768 in all
- w_out: bfloat16 [2048, 4096], P('tp', 'kv'), may hold values from -0.1875 to 0.1875
- gain_mixer: bfloat16 [4096], replicated, may hold values from 0.099609375 to 1.8984375
- w_up: bfloat16 [4096, 16384], P('kv', 'tp'), may hold values from -0.09375 to 0.09375
- w_down: bfloat16 [16384, 4096], P('tp', 'kv'), may hold values from -0.0625 to 0.0625
Outputs:
- output: bfloat16 [16, 4096], P(None, ('kv', 'tp'))
The draws below stay inside these ranges and needn't reach their ends.
Inputs may be any that keep to these rules, and one draw needn't show every extreme that they name: One sequence has all 4096 positions live; the lengths add up to half of 16 times 4096. `gates_cache`: along positions each entry is the running sum of per-position log forget gates up to and including that position, so the values never rise.
All inputs are finite; a program needn't handle non-finite values.
Results may differ from the reference program's by a relative error of at most 0.017.
Values may be sent and summed in bfloat16 or wider, within the bound.
A program may use at most 128 MiB of HBM per device.

```python
import math
import jax
import jax.numpy as jnp
import numpy as np
from jax import lax

D = 4096
ATTENDER_NUMBER = 32
FF = 16384
BATCH_STRINGS = 16
STORED_POSITIONS = 4096
QW = 2048
N_KV = 8
N_TP = 4


def draw_gates_cache(key, part):
    split_prng_material = jax.random.split(jax.random.fold_in(key, 7), 6)
    share = 0.5
    slow_heads = jax.random.uniform(split_prng_material[0], (ATTENDER_NUMBER,)) < share
    slow_rate = jnp.exp(jax.random.uniform(split_prng_material[1], (ATTENDER_NUMBER,), minval=jnp.log(0.2), maxval=jnp.log(0.8))) / STORED_POSITIONS
    fast_rate = jnp.exp(jax.random.uniform(split_prng_material[2], (ATTENDER_NUMBER,), minval=jnp.log(0.01), maxval=jnp.log(1.0 / 30.0)))
    rate = jnp.where(slow_heads, slow_rate, fast_rate)
    factor = jnp.exp(jax.random.uniform(split_prng_material[3], (BATCH_STRINGS, ATTENDER_NUMBER, N_KV), minval=-0.7, maxval=0.7))
    factor = jnp.repeat(factor, STORED_POSITIONS // N_KV, axis=-1)
    rough = jax.random.uniform(split_prng_material[4], (BATCH_STRINGS, ATTENDER_NUMBER, STORED_POSITIONS), minval=0.5, maxval=1.5)
    decoding_logarithmic_decays = -rate[None, :, None] * factor * rough
    draw_filled_extents = jax.random.uniform(split_prng_material[5], (2, BATCH_STRINGS, ATTENDER_NUMBER, STORED_POSITIONS))
    filled_extents = jnp.where(draw_filled_extents[0] < 3.0 / STORED_POSITIONS, jnp.log(0.5 + 0.3 * draw_filled_extents[1]), 0.0)
    return jnp.cumsum(decoding_logarithmic_decays + filled_extents, axis=-1).astype(jnp.float32)


def draw_keys_cache(key, part):
    split_prng_material = jax.random.split(jax.random.fold_in(key, 11), 1)
    base = jnp.clip(jax.random.normal(split_prng_material[0], (BATCH_STRINGS, STORED_POSITIONS, QW), jnp.float32), -6.0, 6.0)
    return base.astype(jnp.bfloat16)


def with_spikes(array, key, source, target, parts, factor):
    owner, partner = [(jnp.arange(array.shape[dim]) // (array.shape[dim] // parts)).reshape([-1 if axis == dim else 1 for axis in range(array.ndim)]) for dim in (source, target)]
    chosen = jax.random.permutation(key, parts)[partner]
    strong = (owner == chosen) | (owner == (partner + parts // 2) % parts)
    return jnp.where(strong, factor * array, array)


def level_of(rng, shape, pieces, least, top_value):
    level, own = 1.0, jax.random.fold_in(rng, 6)
    for position, parts in pieces:
        draws = jnp.exp(jax.random.uniform(jax.random.fold_in(own, position), (parts,), jnp.float32, least / len(pieces), top_value / len(pieces)))
        level = level * jnp.repeat(draws, shape[position] // parts).reshape([-1 if axis == position else 1 for axis in range(len(shape))])
    return level


def profile(number_of, total, most, slope):
    weights = [(1 << 20) // math.isqrt(grade ** slope) + 1 for grade in range(2, number_of + 1)]
    rest, counts = total - most - (number_of - 1), [1] * (number_of - 1)
    while rest > 0:
        candidates = [i for i in range(number_of - 1) if counts[i] < most]
        mass, left = sum([weights[i] for i in candidates]), rest
        for i in candidates:
            more = min(most - counts[i], max(1, left * weights[i] // mass), rest)
            counts[i] = counts[i] + more
            rest = rest - more
    return np.array([most] + counts)


def ragged_sizes(stream_key, number_of, total, bound, lean):
    if number_of == 2:
        one = jax.random.randint(stream_key, (), max(1, total - bound), min(bound, total - 1) + 1)
        return jnp.stack([one, total - one])
    sizes = jnp.asarray(profile(number_of, total, bound, lean), jnp.int32)
    couples = (number_of - 1) // 2
    giver, sink = sizes[1:1 + 2 * couples:2], sizes[2:2 + 2 * couples:2]
    slack = jnp.minimum(giver - 1, bound - sink)
    moved = jax.random.randint(jax.random.fold_in(stream_key, 1), (couples,), 0, 1 << 20) % (slack + 1)
    sizes = sizes.at[1:1 + 2 * couples:2].set(giver - moved).at[2:2 + 2 * couples:2].set(sink + moved)
    return sizes[jax.random.permutation(jax.random.fold_in(stream_key, 2), number_of)]


def normal_values(own_key, shape, width, most, shards=(), kind=jnp.bfloat16):
    result = width * jax.random.normal(own_key, shape, jnp.float32)
    if shards:
        result = result * level_of(own_key, shape, shards, -0.22, 0.18)
    return jnp.clip(result, -most, most).astype(kind)


def heavy_noise(rng, extent, width, reach, cuts, heavy, kind=jnp.bfloat16):
    drawn = width * jax.random.normal(rng, extent, jnp.float32)
    if cuts:
        drawn = drawn * level_of(rng, extent, cuts, -0.22, 0.18)
    return jnp.clip(with_spikes(drawn, jax.random.fold_in(rng, 3), *heavy), -reach, reach).astype(kind)


def setup_inputs(seed: int = 0) -> dict:
    streams_of = jax.random.split(jax.random.key(seed), 16)
    return {
        "tokens": normal_values(streams_of[0], (BATCH_STRINGS, D), 1.0, 6.0, ((1, 32),)),
        "gain_attn": jnp.clip(1.0 + 0.18 * jax.random.normal(streams_of[1], (D,), jnp.float32), 0.099609375, 1.8984375).astype(jnp.bfloat16),
        "w_query": normal_values(streams_of[2], (D, QW), D ** -0.5, 0.09375, ((0, 8), (1, 4))),
        "w_key": normal_values(streams_of[3], (D, QW), D ** -0.5, 0.09375, ((0, 8), (1, 4))),
        "w_value": normal_values(streams_of[4], (D, QW), D ** -0.5, 0.09375, ((0, 8), (1, 4))),
        "w_forget": normal_values(streams_of[5], (D, ATTENDER_NUMBER), D ** -0.5, 0.09375),
        "forget_bias": jnp.clip(jax.random.uniform(streams_of[6], (ATTENDER_NUMBER,), jnp.float32, -2.0, 2.0), -2.0, 2.0),
        "keys_cache": draw_keys_cache(jax.random.fold_in(streams_of[15], 71), 0),
        "values_cache": normal_values(streams_of[8], (BATCH_STRINGS, STORED_POSITIONS, QW), 1.0, 6.0, ((1, 8), (2, 4))),
        "gates_cache": draw_gates_cache(jax.random.fold_in(streams_of[15], 71), 0),
        "lengths": ragged_sizes(streams_of[10], BATCH_STRINGS, BATCH_STRINGS * STORED_POSITIONS // 2, STORED_POSITIONS, 2).astype(jnp.int32),
        "w_out": heavy_noise(streams_of[11], (QW, D), QW ** -0.5, 0.1875, ((0, 4), (1, 8)), (0, 1, 8, 2.0)),
        "gain_mixer": jnp.clip(1.0 + 0.18 * jax.random.normal(streams_of[12], (D,), jnp.float32), 0.099609375, 1.8984375).astype(jnp.bfloat16),
        "w_up": normal_values(streams_of[13], (D, FF), D ** -0.5, 0.09375, ((0, 8), (1, 4))),
        "w_down": heavy_noise(streams_of[14], (FF, D), FF ** -0.5, 0.0625, ((0, 4), (1, 8)), (0, 1, 8, 2.0)),
    }


norm_eps = 1e-06

def attend_one(items):
    query, keys, values, gates, length, forget_log, new_key, new_value = items
    heads = gates.shape[0]
    query_f = query.reshape(heads, -1).astype(jnp.float32)
    scale = query_f.shape[-1] ** (-0.5)
    keys_f = keys.reshape(keys.shape[0], heads, -1).astype(jnp.float32)
    values_f = values.reshape(values.shape[0], heads, -1).astype(jnp.float32)
    scores = jnp.einsum('hd,lhd->hl', query_f, keys_f) * scale
    last_gate = lax.dynamic_slice_in_dim(gates, (length - 1).astype(jnp.int32), 1, 1)[:, 0]
    logits = scores + (last_gate + forget_log)[:, None] - gates
    valid = jnp.arange(gates.shape[1], dtype=jnp.int32) < length
    logits = jnp.where(valid[None, :], logits, -jnp.inf)
    own = lax.optimization_barrier(jnp.sum(query_f * new_key.reshape(heads, -1).astype(jnp.float32), axis=-1)) * scale
    top = jnp.maximum(lax.optimization_barrier(jnp.max(logits, axis=-1)), own)
    weights = jnp.exp(logits - top[:, None])
    own_weight = jnp.exp(own - top)
    total = lax.optimization_barrier(jnp.sum(weights, axis=-1)) + own_weight
    rounded = weights.astype(jnp.bfloat16).astype(jnp.float32)
    summed = jnp.einsum('hl,lhd->hd', rounded, values_f)
    summed = summed + own_weight[:, None] * new_value.reshape(heads, -1).astype(jnp.float32)
    return (summed / total[:, None]).reshape(-1).astype(jnp.bfloat16)

def reference(tokens, gain_attn, w_query, w_key, w_value, w_forget, forget_bias, keys_cache, values_cache, gates_cache, lengths, w_out, gain_mixer, w_up, w_down):
    tokens_f = tokens.astype(jnp.float32)
    attn_scale = lax.rsqrt(lax.optimization_barrier(jnp.mean(tokens_f * tokens_f, axis=-1, keepdims=True)) + norm_eps)
    scaled_in = (tokens_f * gain_attn.astype(jnp.float32)).astype(jnp.bfloat16)
    query = (attn_scale * jnp.dot(scaled_in, w_query, preferred_element_type=jnp.float32)).astype(jnp.bfloat16)
    new_key = (attn_scale * jnp.dot(scaled_in, w_key, preferred_element_type=jnp.float32)).astype(jnp.bfloat16)
    new_value = (attn_scale * jnp.dot(scaled_in, w_value, preferred_element_type=jnp.float32)).astype(jnp.bfloat16)
    forget_log = jax.nn.log_sigmoid(attn_scale * jnp.dot(scaled_in, w_forget, preferred_element_type=jnp.float32) + forget_bias)
    mixed = lax.map(attend_one, (query, keys_cache, values_cache, gates_cache, lengths.astype(jnp.int32), forget_log, new_key, new_value))
    seqs = tokens.shape[0]
    group_width = mixed.shape[1] // N_TP
    mixed_groups = mixed.reshape(seqs, N_TP, group_width).astype(jnp.float32)
    out_groups = w_out.reshape(N_TP, group_width, -1).astype(jnp.float32)
    head_parts = jnp.einsum('bgk,gkd->gbd', mixed_groups, out_groups).astype(jnp.bfloat16)
    head_parts = lax.optimization_barrier(head_parts).astype(jnp.float32)
    residual = (tokens_f + lax.optimization_barrier(jnp.sum(head_parts, axis=0))).astype(jnp.bfloat16)
    residual_f = residual.astype(jnp.float32)
    mixer_scale = lax.rsqrt(lax.optimization_barrier(jnp.mean(residual_f * residual_f, axis=-1, keepdims=True)) + norm_eps)
    scaled_mid = (residual_f * gain_mixer.astype(jnp.float32)).astype(jnp.bfloat16)
    upward = jax.nn.relu(mixer_scale * jnp.dot(scaled_mid, w_up, preferred_element_type=jnp.float32))
    hidden = (upward * upward).astype(jnp.bfloat16)
    down = jnp.dot(hidden, w_down, preferred_element_type=jnp.float32)
    return (residual_f + down).astype(jnp.bfloat16)
```

```python
import functools

import jax
import jax.numpy as jnp
from jax import lax
from jax.experimental import pallas as pl
from jax.experimental.pallas import tpu as pltpu
from jax.sharding import PartitionSpec as P

norm_eps = 1e-06


def combined_all(value, axis, join):
    pieces = jax.tree.map(lambda part: lax.all_gather(part, axis), value)
    head = jax.tree.map(lambda part: part[0], pieces)
    tail = jax.tree.map(lambda part: part[1:], pieces)
    total, _ = lax.scan(lambda total, section: (join(total, section), None), head, tail)
    return total


def combine_parts(earlier, later):
    top = jnp.maximum(earlier[0], later[0])
    early_factor = jnp.exp(earlier[0] - top)
    late_factor = jnp.exp(later[0] - top)
    totals = earlier[1] * early_factor + later[1] * late_factor
    summed = earlier[2] * early_factor[..., None] + later[2] * late_factor[..., None]
    return (top, totals, summed, earlier[3] + later[3])


def channel_mix(residual, gain_mixer, w_up, w_down, kv_index):
    width = gain_mixer.shape[0]
    block_start = kv_index * w_up.shape[0]
    piece = lax.all_gather(residual, "tp", axis=1, tiled=True)
    piece_f = piece.astype(jnp.float32)
    gain_part = lax.dynamic_slice_in_dim(gain_mixer, block_start, piece.shape[1], 0).astype(
        jnp.float32
    )
    scaled = (piece_f * gain_part).astype(jnp.bfloat16)
    upward = jnp.dot(scaled, w_up, preferred_element_type=jnp.float32)
    upward, squares = (upward, jnp.sum(piece_f * piece_f, axis=-1))
    up_total, square_total = lax.psum((upward, squares), "kv")
    mixer_scale = lax.rsqrt(square_total / width + norm_eps)
    active = jax.nn.relu(mixer_scale[:, None] * up_total)
    hidden = (active * active).astype(jnp.bfloat16)
    down = jnp.dot(hidden, w_down, preferred_element_type=jnp.float32)
    return lax.psum_scatter(down, "tp", scatter_dimension=1, tiled=True)


def shards(
    tokens,
    gain_attn,
    w_query,
    w_key,
    w_value,
    w_forget,
    forget_bias,
    keys_cache,
    values_cache,
    gates_cache,
    lengths,
    w_out,
    gain_mixer,
    w_up,
    w_down,
):
    kv_index = lax.axis_index("kv")
    tp_index = lax.axis_index("tp")
    row_block = w_query.shape[0]
    heads_here = gates_cache.shape[1]
    width = gain_attn.shape[0]
    row_start = kv_index * row_block
    head_start = tp_index * heads_here
    block_raw = lax.all_gather(tokens, "tp", axis=1, tiled=True)
    block_f = block_raw.astype(jnp.float32)
    gain_block = lax.dynamic_slice_in_dim(gain_attn, row_start, row_block, 0).astype(jnp.float32)
    block = (block_f * gain_block).astype(jnp.bfloat16)
    forget_block = lax.dynamic_slice(w_forget, (row_start, head_start), (row_block, heads_here))
    part_query = jnp.dot(block, w_query, preferred_element_type=jnp.float32)
    part_key = jnp.dot(block, w_key, preferred_element_type=jnp.float32)
    part_value = jnp.dot(block, w_value, preferred_element_type=jnp.float32)
    part_gate = jnp.dot(block, forget_block, preferred_element_type=jnp.float32)
    part_squares = jnp.sum(block_f * block_f, axis=-1)
    sum_query, sum_key, sum_value, sum_gate, squares = lax.psum(
        (part_query, part_key, part_value, part_gate, part_squares), "kv"
    )
    attn_scale = lax.rsqrt(squares / width + norm_eps)[:, None]
    gate_logit = attn_scale * sum_gate
    query = (attn_scale * sum_query).astype(jnp.bfloat16)
    new_key = (attn_scale * sum_key).astype(jnp.bfloat16)
    new_value = (attn_scale * sum_value).astype(jnp.bfloat16)
    bias_here = lax.dynamic_slice_in_dim(forget_bias, head_start, heads_here, 0)
    forget_log = jax.nn.log_sigmoid(gate_logit + bias_here)
    seqs = tokens.shape[0]
    positions_here = keys_cache.shape[1]
    query_heads = query.reshape(seqs, heads_here, -1)
    head_size = query_heads.shape[-1]
    keys_heads = keys_cache.reshape(seqs, positions_here, heads_here, head_size)
    values_heads = values_cache.reshape(seqs, positions_here, heads_here, head_size)
    scores = jnp.einsum(
        "bhd,bphd->bhp", query_heads, keys_heads, preferred_element_type=jnp.float32
    )
    logits = scores * head_size ** (-0.5) - gates_cache
    positions = kv_index * positions_here + jnp.arange(positions_here, dtype=jnp.int32)
    valid = (positions[None, :] < lengths[:, None])[:, None, :]
    local_top = jnp.max(jnp.where(valid, logits, -1e30), axis=-1)
    weights = jnp.where(valid, jnp.exp(logits - local_top[..., None]), 0.0)
    local_total = jnp.sum(weights, axis=-1)
    local_sum = jnp.einsum(
        "bhp,bphd->bhd",
        weights.astype(jnp.bfloat16),
        values_heads,
        preferred_element_type=jnp.float32,
    )
    at_last = (positions[None, :] == lengths[:, None] - 1)[:, None, :]
    last_local = jnp.sum(jnp.where(at_last, gates_cache, 0.0), axis=-1)
    top, totals, summed, last_gate = combined_all(
        (local_top, local_total, local_sum, last_local), "kv", combine_parts
    )
    top = top + last_gate + forget_log
    own = jnp.sum(
        query_heads.astype(jnp.float32) * new_key.reshape(seqs, heads_here, -1).astype(jnp.float32),
        axis=-1,
    ) * head_size ** (-0.5)
    overall = jnp.maximum(top, own)
    cache_factor = jnp.exp(top - overall)
    own_weight = jnp.exp(own - overall)
    denominator = totals * cache_factor + own_weight
    numerator = summed * cache_factor[..., None] + own_weight[..., None] * new_value.reshape(
        seqs, heads_here, -1
    ).astype(jnp.float32)
    mixed = (numerator / denominator[..., None]).astype(jnp.bfloat16).reshape(seqs, -1)
    partial_value = jnp.dot(mixed, w_out, preferred_element_type=jnp.float32).astype(jnp.bfloat16)
    attended = lax.psum_scatter(partial_value, "tp", scatter_dimension=1, tiled=True).astype(
        jnp.float32
    )
    residual = (tokens.astype(jnp.float32) + attended).astype(jnp.bfloat16)
    mixer = channel_mix(residual, gain_mixer, w_up, w_down, kv_index)
    return (residual.astype(jnp.float32) + mixer).astype(jnp.bfloat16)


f32, bf16 = jnp.float32, jnp.bfloat16
LANES = 128


def spread_rows(rows, width):
    shape = (rows, width)
    return lax.broadcasted_iota(jnp.int32, shape, 0), lax.broadcasted_iota(jnp.int32, shape, 1)


def to_row(column):
    row, lane = spread_rows(column.shape[0], LANES)
    return jnp.sum(jnp.where(row == lane, column, 0.0), axis=0, keepdims=True)


def to_column(line, count):
    row, lane = spread_rows(count, LANES)
    return jnp.sum(jnp.where(row == lane, line, 0.0), axis=-1, keepdims=True)


def fused(
    n_kv,
    n_tp,
    tokens,
    gain_attn_any,
    forget_bias_any,
    lengths_any,
    gain_mixer_any,
    w_query,
    w_key,
    w_value,
    w_forget,
    keys_cache,
    values_cache,
    gates_cache,
    w_out,
    w_up,
    w_down,
    out,
    gain_attn,
    gain_mixer,
    forget_bias,
    lengths,
    wq,
    wk,
    wv,
    wf,
    keys,
    values,
    gates,
    wo,
    wu,
    wd,
    bias_t,
    tok_all,
    q_all,
    p_send,
    p_all,
    s_all,
    g_all,
    t_all,
    n_all,
    a_all,
    o_all,
    u_send,
    u_all,
    h_all,
    f_send,
    f_all,
    query,
    coef,
    res,
    load_sem,
    kv_out,
    kv_in,
    tp_out,
    tp_in,
    u_out,
    u_in,
    h_out,
    h_in,
):
    kv, tp = lax.axis_index("kv"), lax.axis_index("tp")
    seqs, piece = tok_all.shape[1:]
    rows, cols = wq.shape
    positions = keys.shape[1]
    heads = gates.shape[1]
    all_heads = wf.shape[0]
    size = cols // heads
    mine = seqs // n_kv
    width = gain_attn.shape[0]
    q_parts, q_rows = q_all.shape[1:3]
    a_parts, a_rows = a_all.shape[1:3]
    n_own, chunks = h_all.shape[:2]
    part = h_all.shape[3]
    first = n_kv // 4
    upper = kv // n_own
    is_owner = jnp.logical_and(kv >= first, kv < first + n_own)
    never = -3e38

    barrier = pltpu.get_barrier_semaphore()
    for j in range(1, n_tp):
        pl.semaphore_signal(
            barrier,
            inc=1,
            device_id=(kv, lax.rem(tp + j, n_tp)),
            device_id_type=pl.DeviceIdType.MESH,
        )
    turn = 2 * upper - 1

    def kv_peer(j):
        return lax.rem(kv + turn * j + n_kv, n_kv)

    for j in range(1, n_kv):
        pl.semaphore_signal(
            barrier,
            inc=1,
            device_id=(kv_peer(j), tp),
            device_id_type=pl.DeviceIdType.MESH,
        )

    row_at = pl.multiple_of(kv * rows, rows)
    sources = [
        (tokens, tok_all.at[tp]),
        (lengths_any, lengths),
        (gain_attn_any, gain_attn),
        (forget_bias_any, forget_bias),
        (gain_mixer_any, gain_mixer),
        (gates_cache, gates),
        (w_query, wq),
        (w_forget.at[:, pl.ds(row_at, rows)], wf),
        (w_key, wk),
        (w_value, wv),
        (keys_cache, keys),
        (values_cache, values),
        (w_out, wo),
        (w_up, wu),
        (w_down, wd),
    ]
    loads = [pltpu.make_async_copy(a, b, load_sem.at[i]) for i, (a, b) in enumerate(sources)]
    for load in loads:
        load.start()
    (
        ld_tok,
        ld_len,
        ld_ga,
        ld_bias,
        ld_gm,
        ld_gates,
        ld_q,
        ld_f,
        ld_k,
        ld_v,
        ld_keys,
        ld_values,
        ld_o,
        ld_u,
        ld_d,
    ) = loads

    def remote(source, target, out_sem, in_sem, device):
        return pltpu.make_async_remote_copy(
            src_ref=source,
            dst_ref=target,
            send_sem=out_sem,
            recv_sem=in_sem,
            device_id=device,
            device_id_type=pl.DeviceIdType.MESH,
        )

    pending = []

    def flush():
        for copy in pending:
            copy.wait_send()
        pending.clear()

    def start(copy):
        copy.start()
        pending.append(copy)

    def spread_kv(phase, slot):
        for j in range(1, n_kv):
            start(
                remote(
                    slot(kv),
                    slot(kv),
                    kv_out.at[phase, j],
                    kv_in.at[phase, kv],
                    (kv_peer(j), tp),
                )
            )

    def from_kv(phase, j, slot):
        peer = lax.rem(kv - turn * j + n_kv, n_kv)
        remote(
            slot(peer), slot(peer), kv_out.at[phase, j], kv_in.at[phase, peer], (peer, tp)
        ).wait_recv()

    def gather_kv(phase, slot):
        for j in range(1, n_kv):
            from_kv(phase, j, slot)

    def spread_tp(phase, slot):
        for j in range(1, n_tp):
            start(
                remote(
                    slot(tp),
                    slot(tp),
                    tp_out.at[phase, j],
                    tp_in.at[phase, tp],
                    (kv, lax.rem(tp + j, n_tp)),
                )
            )

    def gather_tp(phase, slot):
        for j in range(1, n_tp):
            peer = lax.rem(tp + n_tp - j, n_tp)
            remote(
                slot(peer), slot(peer), tp_out.at[phase, j], tp_in.at[phase, peer], (kv, peer)
            ).wait_recv()

    def total_of(read):
        total = read(0).astype(f32)
        for o in range(1, n_kv):
            total = total + read(o).astype(f32)
        return total

    ld_tok.wait()
    pl.semaphore_wait(barrier, n_kv + n_tp - 2)
    spread_tp(0, lambda t: tok_all.at[t])

    ld_len.wait()
    ld_ga.wait()
    ld_bias.wait()
    ld_gm.wait()
    ld_gates.wait()
    lane_seq = lax.broadcasted_iota(jnp.int32, (1, LANES), 1) // heads
    length_row = jnp.zeros((1, LANES), jnp.int32)
    for b in range(seqs):
        length_row = jnp.where(lane_seq == b, lengths[b], length_row)
    gates_t = jnp.transpose(gates[...].reshape(seqs * heads, positions))
    place = kv * positions + lax.broadcasted_iota(jnp.int32, (positions, LANES), 0)
    bias_t[...] = jnp.where(place < length_row, -gates_t, never)
    last_row = jnp.sum(jnp.where(place == length_row - 1, gates_t, 0.0), axis=0, keepdims=True)
    gain_a = gain_attn[pl.ds(row_at, rows)].astype(f32).reshape(1, rows)
    gain_m = gain_mixer[pl.ds(row_at, rows)].astype(f32).reshape(1, rows)

    gather_tp(0, lambda t: tok_all.at[t])
    tok = jnp.concatenate([tok_all[t] for t in range(n_tp)], axis=1).astype(f32)
    scaled = (tok * gain_a).astype(bf16)
    s_all[0, kv] = to_row(jnp.sum(tok * tok, axis=-1, keepdims=True))
    spread_kv(0, lambda o: s_all.at[0, o])
    ld_q.wait()
    q_part = jnp.dot(scaled, wq[...], preferred_element_type=f32).astype(bf16)
    for c in range(q_parts):
        q_all[kv, c] = q_part[c * q_rows : (c + 1) * q_rows]
    for c in range(q_parts):
        spread_kv(1 + c, lambda o, c=c: q_all.at[o, c])

    ld_k.wait()
    ld_v.wait()
    ld_f.wait()
    part_key = jnp.dot(scaled, wk[...], preferred_element_type=f32)
    part_value = jnp.dot(scaled, wv[...], preferred_element_type=f32)
    for o in range(n_kv):
        at = slice(o * mine, (o + 1) * mine)
        p_send[o, :, :cols] = part_key[at]
        p_send[o, :, cols:] = part_value[at]
    for j in range(1, n_kv):
        peer = kv_peer(j)
        start(
            remote(
                p_send.at[peer],
                p_all.at[kv],
                kv_out.at[P_PHASE, j],
                kv_in.at[P_PHASE, kv],
                (peer, tp),
            )
        )
    p_all[kv] = p_send[kv]

    part_gate = lax.dot_general(
        scaled, wf[...], (((1,), (1,)), ((), ())), preferred_element_type=f32
    )
    tall = jnp.concatenate(
        [part_gate, jnp.broadcast_to(forget_bias[...], (8, all_heads))], axis=0
    )
    head_lane = lax.broadcasted_iota(jnp.int32, tall.shape, 1) - tp * heads
    lane_head = lax.broadcasted_iota(jnp.int32, (1, LANES), 1) % heads
    wide = jnp.zeros((seqs + 8, LANES), f32)
    for h in range(heads):
        column = jnp.sum(jnp.where(head_lane == h, tall, 0.0), axis=-1, keepdims=True)
        wide = jnp.where(lane_head == h, column, wide)
    seq_row = lax.broadcasted_iota(jnp.int32, (seqs, LANES), 0)
    here = seq_row == lane_seq
    g_all[kv, 0:1, :] = jnp.sum(jnp.where(here, wide[:seqs], 0.0), axis=0, keepdims=True)
    g_all[kv, 1:2, :] = last_row
    spread_kv(G_PHASE, lambda o: g_all.at[o])
    bias_row = wide[seqs : seqs + 1]

    gather_kv(0, lambda o: s_all.at[0, o])
    squares = to_column(total_of(lambda o: s_all[0, o]), seqs)
    attn_scale = lax.rsqrt(squares / width + norm_eps)
    query[:, cols:] = jnp.broadcast_to(attn_scale, (seqs, LANES))
    own_block = (
        lax.broadcasted_iota(jnp.int32, (heads, cols), 0)
        == lax.broadcasted_iota(jnp.int32, (heads, cols), 1) // size
    )
    ld_keys.wait()
    scores = jnp.zeros((positions, LANES), f32)
    for c in range(q_parts):
        gather_kv(1 + c, lambda o, c=c: q_all.at[o, c])
        q_here = total_of(lambda o, c=c: q_all[o, c])
        q_here = (attn_scale[c * q_rows : (c + 1) * q_rows] * q_here).astype(bf16).astype(f32)
        query[c * q_rows : (c + 1) * q_rows, :cols] = q_here
        lefts, rights = [], []
        for r in range(q_rows):
            b = c * q_rows + r
            block = jnp.where(own_block, q_here[r : r + 1], 0.0)
            right = [jnp.zeros((b * heads, cols), f32)] if b else []
            right.append(block)
            if b + 1 < seqs:
                right.append(jnp.zeros(((seqs - b - 1) * heads, cols), f32))
            rights.append(jnp.concatenate(right, axis=0).astype(bf16))
            lefts.append(keys[b])
        scores = scores + lax.dot_general(
            jnp.concatenate(lefts, axis=1),
            jnp.concatenate(rights, axis=1),
            (((1,), (1,)), ((), ())),
            preferred_element_type=f32,
        )

    logits = scores * size ** (-0.5) + bias_t[...]
    top = jnp.maximum(jnp.max(logits, axis=0, keepdims=True), -1e30)
    weights = jnp.exp(logits - top)
    t_all[kv, 0:1, :] = top
    t_all[kv, 1:2, :] = jnp.sum(weights, axis=0, keepdims=True)
    spread_kv(T_PHASE, lambda o: t_all.at[o])
    weights = jnp.transpose(weights).astype(bf16)
    ld_values.wait()

    def attend(pair):
        left = weights[pair * 2 * heads : (pair + 1) * 2 * heads]
        found = []
        for r in range(2):
            summed = jnp.dot(left, values[2 * pair + r], preferred_element_type=f32)
            summed = jnp.where(own_block, summed[r * heads : (r + 1) * heads], 0.0)
            found.append(jnp.sum(summed, axis=0, keepdims=True))
        return found

    def own_token():
        gather_kv(P_PHASE, lambda o: p_all.at[o])
        gather_kv(G_PHASE, lambda o: g_all.at[o])
        scale_row = jnp.sum(jnp.where(here, attn_scale, 0.0), axis=0, keepdims=True)
        gate_sum = total_of(lambda o: g_all[o])
        gate_logit = scale_row * gate_sum[0:1] + bias_row
        forget_log = jnp.minimum(gate_logit, 0.0) - jnp.log1p(jnp.exp(-jnp.abs(gate_logit)))
        p_total = total_of(lambda o: p_all[o])
        own_rows = [query[pl.ds(kv * mine + r, 1), :] for r in range(mine)]
        own_query = jnp.concatenate(own_rows, axis=0)
        own_scale = own_query[:, cols : cols + 1]
        new_key = (own_scale * p_total[:, :cols]).astype(bf16).astype(f32)
        n_all[kv, :, :cols] = (own_scale * p_total[:, cols:]).astype(bf16).astype(f32)
        product = own_query[:, :cols] * new_key
        col_head = lax.broadcasted_iota(jnp.int32, (mine, cols), 1) // size
        own = jnp.full((mine, LANES), never, f32)
        own_seq = kv * mine + lax.broadcasted_iota(jnp.int32, (mine, LANES), 0)
        for h in range(heads):
            column = jnp.sum(jnp.where(col_head == h, product, 0.0), axis=-1, keepdims=True)
            at = jnp.logical_and(lane_head == h, lane_seq == own_seq)
            own = jnp.where(at, column * size ** (-0.5), own)
        own = own - jnp.where(lane_seq == own_seq, gate_sum[1:2] + forget_log, 0.0)
        n_all[kv, :, cols:] = own
        spread_kv(N_PHASE, lambda o: n_all.at[o])

    def weigh_parts():
        gather_kv(T_PHASE, lambda o: t_all.at[o])
        gather_kv(N_PHASE, lambda o: n_all.at[o])
        own = jnp.max(n_all[0, :, cols:], axis=0, keepdims=True)
        for o in range(1, n_kv):
            own = jnp.maximum(own, jnp.max(n_all[o, :, cols:], axis=0, keepdims=True))
        tops = [t_all[o, 0:1, :] for o in range(n_kv)] + [own]
        totals = [t_all[o, 1:2, :] for o in range(n_kv)] + [jnp.ones((1, LANES), f32)]
        overall = functools.reduce(jnp.maximum, tops)
        factors = [jnp.exp(one - overall) for one in tops]
        denominator = sum(one * total for one, total in zip(factors, totals))
        stack = jnp.concatenate(
            [jnp.where(here, one / denominator, 0.0) for one in factors], axis=0
        )
        high = stack.astype(bf16)
        low = (stack - high.astype(f32)).astype(bf16)
        lane = lax.broadcasted_iota(jnp.int32, (2 * LANES, cols), 0) % heads
        same = lane == lax.broadcasted_iota(jnp.int32, (2 * LANES, cols), 1) // size
        coef[...] = jnp.dot(
            jnp.concatenate([high, low], axis=1),
            jnp.where(same, 1.0, 0.0).astype(bf16),
            preferred_element_type=f32,
        )

    pairs_per = a_rows // 2
    for c in range(a_parts):
        found = []
        for i in range(pairs_per):
            found.extend(attend(c * pairs_per + i))
        a_all[kv, c] = jnp.concatenate(found, axis=0).astype(bf16)
        spread_kv(A_PHASE + c, lambda o, c=c: a_all.at[o, c])
        if c == 0:
            own_token()
    flush()
    weigh_parts()
    ld_o.wait()
    added = []
    new_values = jnp.concatenate([n_all[o, :, :cols] for o in range(n_kv)], axis=0)
    for c in range(a_parts):
        gather_kv(A_PHASE + c, lambda o, c=c: a_all.at[o, c])
        own_at = n_kv * seqs + c * a_rows
        mixed = coef[own_at : own_at + a_rows] * new_values[c * a_rows : (c + 1) * a_rows]
        for o in range(n_kv):
            at = o * seqs + c * a_rows
            mixed = mixed + coef[at : at + a_rows] * a_all[o, c].astype(f32)
        added.append(mixed)
    mixed = jnp.concatenate(added, axis=0).astype(bf16)
    o_all[tp] = jnp.dot(mixed, wo[...], preferred_element_type=f32).astype(bf16)
    spread_tp(1, lambda t: o_all.at[t])
    ld_u.wait()
    flush()
    gather_tp(1, lambda t: o_all.at[t])
    attended = o_all[0].astype(f32)
    for t in range(1, n_tp):
        attended = attended + o_all[t].astype(f32)
    residual = (tok + attended).astype(bf16).astype(f32)
    for t in range(n_tp):
        res[t] = residual[:, t * piece : (t + 1) * piece]
    scaled_mid = (residual * gain_m).astype(bf16)

    def owner_at(j):
        near = (n_own // 2 + j) % n_own
        return near + upper * (n_own - 1 - 2 * near)

    def elsewhere(m, act):
        pl.when(first + m != kv)(act)

    s_all[1, kv] = to_row(jnp.sum(residual * residual, axis=-1, keepdims=True))

    def square_copy(m):
        return remote(
            s_all.at[1, kv],
            s_all.at[1, kv],
            u_out.at[chunks, m],
            u_in.at[chunks, kv],
            (first + m, tp),
        )

    def up_copy(m, c):
        return remote(
            u_send.at[m, c], u_all.at[kv, c], u_out.at[c, m], u_in.at[c, kv], (first + m, tp)
        )

    for j in range(n_own):
        m = owner_at(j)
        elsewhere(m, lambda m=m: square_copy(m).start())
    for c in range(chunks):
        for j in range(n_own):
            m = owner_at(j)
            at = pl.multiple_of((m * chunks + c) * part, part)
            u_send[m, c] = jnp.dot(
                scaled_mid, wu[:, pl.ds(at, part)], preferred_element_type=f32
            ).astype(bf16)
            elsewhere(m, lambda m=m, c=c: up_copy(m, c).start())

    own_m = kv - first

    def hidden_copy(c, j):
        return remote(
            h_all.at[own_m, c],
            h_all.at[own_m, c],
            h_out.at[c, j],
            h_in.at[c, own_m],
            (kv_peer(j), tp),
        )


    @pl.when(is_owner)
    def _():
        for j in range(1, n_kv):
            peer = lax.rem(kv - turn * j + n_kv, n_kv)
            remote(
                s_all.at[1, peer],
                s_all.at[1, peer],
                u_out.at[chunks, 0],
                u_in.at[chunks, peer],
                (peer, tp),
            ).wait_recv()
        squares = to_column(total_of(lambda o: s_all[1, o]), seqs)
        mixer_scale = lax.rsqrt(squares / width + norm_eps)
        for c in range(chunks):
            total = u_send[own_m, c].astype(f32)
            for j in range(1, n_kv):
                peer = lax.rem(kv - turn * j + n_kv, n_kv)
                remote(
                    u_all.at[peer, c],
                    u_all.at[peer, c],
                    u_out.at[c, 0],
                    u_in.at[c, peer],
                    (peer, tp),
                ).wait_recv()
                total = total + u_all[peer, c].astype(f32)
            active = jnp.maximum(mixer_scale * total, 0.0)
            h_all[own_m, c] = (active * active).astype(bf16)
            for j in range(1, n_kv):
                hidden_copy(c, j).start()

    ld_d.wait()
    for c in range(chunks):
        for j in range(n_own):
            m = owner_at(j)
            elsewhere(m, lambda m=m, c=c: up_copy(m, c).wait_send())
    for j in range(n_own):
        m = owner_at(j)
        elsewhere(m, lambda m=m: square_copy(m).wait_send())

    down = jnp.zeros((seqs, rows), f32)
    for c in range(chunks):
        for j in reversed(range(n_own)):
            m = owner_at(j)

            def arrive(m=m, c=c):
                remote(
                    h_all.at[m, c],
                    h_all.at[m, c],
                    h_out.at[c, 0],
                    h_in.at[c, m],
                    (first + m, tp),
                ).wait_recv()

            elsewhere(m, arrive)
            at = pl.multiple_of((m * chunks + c) * part, part)
            down = down + jnp.dot(
                h_all[m, c], wd[pl.ds(at, part), :], preferred_element_type=f32
            )
    for t in range(n_tp):
        f_send[t] = down[:, t * piece : (t + 1) * piece].astype(bf16)
    for j in range(1, n_tp):
        peer = lax.rem(tp + j, n_tp)
        start(
            remote(
                f_send.at[peer], f_all.at[tp], tp_out.at[2, j], tp_in.at[2, tp], (kv, peer)
            )
        )
    f_all[tp] = f_send[tp]

    @pl.when(is_owner)
    def _():
        for c in range(chunks):
            for j in range(1, n_kv):
                hidden_copy(c, j).wait_send()

    flush()
    gather_tp(2, lambda t: f_all.at[t])
    mixer = f_all[0].astype(f32)
    for t in range(1, n_tp):
        mixer = mixer + f_all[t].astype(f32)
    out[...] = (res[tp] + mixer).astype(bf16)


Q_PARTS = 2
A_PARTS = 2
CHUNKS = 2
P_PHASE = 1 + Q_PARTS
G_PHASE = P_PHASE + 1
T_PHASE = G_PHASE + 1
N_PHASE = T_PHASE + 1
A_PHASE = N_PHASE + 1
PHASES = A_PHASE + A_PARTS


def layer(n_kv, n_tp, *arrays):
    (
        tokens,
        gain_attn,
        w_query,
        w_key,
        w_value,
        w_forget,
        forget_bias,
        keys_cache,
        values_cache,
        gates_cache,
        lengths,
        w_out,
        gain_mixer,
        w_up,
        w_down,
    ) = arrays
    seqs, piece = tokens.shape
    rows, cols = w_query.shape
    positions = keys_cache.shape[1]
    heads = gates_cache.shape[1]
    all_heads = w_forget.shape[1]
    n_own = n_kv // 2
    part = w_up.shape[1] // max(n_own * CHUNKS, 1)
    fits = (
        n_kv % 4 == 0
        and n_tp > 1
        and seqs % n_kv == 0
        and seqs * heads == LANES
        and heads % 8 == 0
        and seqs % (8 * max(Q_PARTS, A_PARTS)) == 0
        and piece % LANES == 0
        and cols % LANES == 0
        and positions % LANES == 0
        and part % LANES == 0
        and w_up.shape[1] == part * n_own * CHUNKS
        and all_heads <= LANES
        and w_out.shape == (cols, rows)
        and rows == n_tp * piece
    )
    if not fits:
        return shards(*arrays)
    mine = seqs // n_kv
    vmem = pl.BlockSpec(memory_space=pltpu.VMEM)
    anywhere = pl.BlockSpec(memory_space=pl.ANY)
    bias = forget_bias.reshape(1, -1)

    def like(x):
        return pltpu.VMEM(x.shape, x.dtype)

    return pl.pallas_call(
        functools.partial(fused, n_kv, n_tp),
        out_shape=jax.ShapeDtypeStruct((seqs, piece), bf16),
        in_specs=[anywhere] * 15,
        out_specs=vmem,
        scratch_shapes=[
            like(gain_attn),
            like(gain_mixer),
            like(bias),
            pltpu.SMEM(lengths.shape, lengths.dtype),
            like(w_query),
            like(w_key),
            like(w_value),
            pltpu.VMEM((all_heads, rows), bf16),
            like(keys_cache),
            like(values_cache),
            like(gates_cache),
            like(w_out),
            like(w_up),
            like(w_down),
            pltpu.VMEM((positions, LANES), f32),
            pltpu.VMEM((n_tp, seqs, piece), bf16),
            pltpu.VMEM((n_kv, Q_PARTS, seqs // Q_PARTS, cols), bf16),
            pltpu.VMEM((n_kv, mine, 2 * cols), f32),
            pltpu.VMEM((n_kv, mine, 2 * cols), f32),
            pltpu.VMEM((2, n_kv, 1, LANES), f32),
            pltpu.VMEM((n_kv, 2, LANES), f32),
            pltpu.VMEM((n_kv, 2, LANES), f32),
            pltpu.VMEM((n_kv, mine, cols + LANES), f32),
            pltpu.VMEM((n_kv, A_PARTS, seqs // A_PARTS, cols), bf16),
            pltpu.VMEM((n_tp, seqs, rows), bf16),
            pltpu.VMEM((n_own, CHUNKS, seqs, part), bf16),
            pltpu.VMEM((n_kv, CHUNKS, seqs, part), bf16),
            pltpu.VMEM((n_own, CHUNKS, seqs, part), bf16),
            pltpu.VMEM((n_tp, seqs, piece), bf16),
            pltpu.VMEM((n_tp, seqs, piece), bf16),
            pltpu.VMEM((seqs, cols + LANES), f32),
            pltpu.VMEM(((n_kv + 1) * seqs, cols), f32),
            pltpu.VMEM((n_tp, seqs, piece), f32),
            pltpu.SemaphoreType.DMA((15,)),
            pltpu.SemaphoreType.DMA((PHASES, n_kv)),
            pltpu.SemaphoreType.DMA((PHASES, n_kv)),
            pltpu.SemaphoreType.DMA((3, n_tp)),
            pltpu.SemaphoreType.DMA((3, n_tp)),
            pltpu.SemaphoreType.DMA((CHUNKS + 1, n_own)),
            pltpu.SemaphoreType.DMA((CHUNKS + 1, n_kv)),
            pltpu.SemaphoreType.DMA((CHUNKS, n_kv)),
            pltpu.SemaphoreType.DMA((CHUNKS, n_own)),
        ],
        compiler_params=pltpu.CompilerParams(
            collective_id=0, has_side_effects=True, vmem_limit_bytes=VMEM_LIMIT
        ),
    )(
        tokens,
        gain_attn,
        bias,
        lengths,
        gain_mixer,
        w_query,
        w_key,
        w_value,
        w_forget.T,
        keys_cache,
        values_cache,
        gates_cache,
        w_out,
        w_up,
        w_down,
    )


VMEM_LIMIT = 60 * 1024 * 1024


def solution(mesh):
    return jax.shard_map(
        functools.partial(layer, mesh.shape["kv"], mesh.shape["tp"]),
        mesh=mesh,
        in_specs=(
            P(None, ("kv", "tp")),
            P(),
            P("kv", "tp"),
            P("kv", "tp"),
            P("kv", "tp"),
            P(),
            P(),
            P(None, "kv", "tp"),
            P(None, "kv", "tp"),
            P(None, "tp", "kv"),
            P(),
            P("tp", "kv"),
            P(),
            P("kv", "tp"),
            P("tp", "kv"),
        ),
        out_specs=P(None, ("kv", "tp")),
        check_vma=False,
    )
```

```python
import functools

import jax
import jax.numpy as jnp
from jax import lax
from jax.experimental import pallas as pl
from jax.experimental.pallas import tpu as pltpu
from jax.sharding import PartitionSpec as P

norm_eps = 1e-06


def combined_all(value, axis, join):
    pieces = jax.tree.map(lambda part: lax.all_gather(part, axis), value)
    head = jax.tree.map(lambda part: part[0], pieces)
    tail = jax.tree.map(lambda part: part[1:], pieces)
    total, _ = lax.scan(lambda total, section: (join(total, section), None), head, tail)
    return total


def combine_parts(earlier, later):
    top = jnp.maximum(earlier[0], later[0])
    early_factor = jnp.exp(earlier[0] - top)
    late_factor = jnp.exp(later[0] - top)
    totals = earlier[1] * early_factor + later[1] * late_factor
    summed = earlier[2] * early_factor[..., None] + later[2] * late_factor[..., None]
    return (top, totals, summed, earlier[3] + later[3])


def channel_mix(residual, gain_mixer, w_up, w_down, kv_index):
    width = gain_mixer.shape[0]
    block_start = kv_index * w_up.shape[0]
    piece = lax.all_gather(residual, "tp", axis=1, tiled=True)
    piece_f = piece.astype(jnp.float32)
    gain_part = lax.dynamic_slice_in_dim(gain_mixer, block_start, piece.shape[1], 0).astype(
        jnp.float32
    )
    scaled = (piece_f * gain_part).astype(jnp.bfloat16)
    upward = jnp.dot(scaled, w_up, preferred_element_type=jnp.float32)
    upward, squares = (upward, jnp.sum(piece_f * piece_f, axis=-1))
    up_total, square_total = lax.psum((upward, squares), "kv")
    mixer_scale = lax.rsqrt(square_total / width + norm_eps)
    active = jax.nn.relu(mixer_scale[:, None] * up_total)
    hidden = (active * active).astype(jnp.bfloat16)
    down = jnp.dot(hidden, w_down, preferred_element_type=jnp.float32)
    return lax.psum_scatter(down, "tp", scatter_dimension=1, tiled=True)


def shards(
    tokens,
    gain_attn,
    w_query,
    w_key,
    w_value,
    w_forget,
    forget_bias,
    keys_cache,
    values_cache,
    gates_cache,
    lengths,
    w_out,
    gain_mixer,
    w_up,
    w_down,
):
    kv_index = lax.axis_index("kv")
    tp_index = lax.axis_index("tp")
    row_block = w_query.shape[0]
    heads_here = gates_cache.shape[1]
    width = gain_attn.shape[0]
    row_start = kv_index * row_block
    head_start = tp_index * heads_here
    block_raw = lax.all_gather(tokens, "tp", axis=1, tiled=True)
    block_f = block_raw.astype(jnp.float32)
    gain_block = lax.dynamic_slice_in_dim(gain_attn, row_start, row_block, 0).astype(jnp.float32)
    block = (block_f * gain_block).astype(jnp.bfloat16)
    forget_block = lax.dynamic_slice(w_forget, (row_start, head_start), (row_block, heads_here))
    part_query = jnp.dot(block, w_query, preferred_element_type=jnp.float32)
    part_key = jnp.dot(block, w_key, preferred_element_type=jnp.float32)
    part_value = jnp.dot(block, w_value, preferred_element_type=jnp.float32)
    part_gate = jnp.dot(block, forget_block, preferred_element_type=jnp.float32)
    part_squares = jnp.sum(block_f * block_f, axis=-1)
    sum_query, sum_key, sum_value, sum_gate, squares = lax.psum(
        (part_query, part_key, part_value, part_gate, part_squares), "kv"
    )
    attn_scale = lax.rsqrt(squares / width + norm_eps)[:, None]
    gate_logit = attn_scale * sum_gate
    query = (attn_scale * sum_query).astype(jnp.bfloat16)
    new_key = (attn_scale * sum_key).astype(jnp.bfloat16)
    new_value = (attn_scale * sum_value).astype(jnp.bfloat16)
    bias_here = lax.dynamic_slice_in_dim(forget_bias, head_start, heads_here, 0)
    forget_log = jax.nn.log_sigmoid(gate_logit + bias_here)
    seqs = tokens.shape[0]
    positions_here = keys_cache.shape[1]
    query_heads = query.reshape(seqs, heads_here, -1)
    head_size = query_heads.shape[-1]
    keys_heads = keys_cache.reshape(seqs, positions_here, heads_here, head_size)
    values_heads = values_cache.reshape(seqs, positions_here, heads_here, head_size)
    scores = jnp.einsum(
        "bhd,bphd->bhp", query_heads, keys_heads, preferred_element_type=jnp.float32
    )
    logits = scores * head_size ** (-0.5) - gates_cache
    positions = kv_index * positions_here + jnp.arange(positions_here, dtype=jnp.int32)
    valid = (positions[None, :] < lengths[:, None])[:, None, :]
    local_top = jnp.max(jnp.where(valid, logits, -1e30), axis=-1)
    weights = jnp.where(valid, jnp.exp(logits - local_top[..., None]), 0.0)
    local_total = jnp.sum(weights, axis=-1)
    local_sum = jnp.einsum(
        "bhp,bphd->bhd",
        weights.astype(jnp.bfloat16),
        values_heads,
        preferred_element_type=jnp.float32,
    )
    at_last = (positions[None, :] == lengths[:, None] - 1)[:, None, :]
    last_local = jnp.sum(jnp.where(at_last, gates_cache, 0.0), axis=-1)
    top, totals, summed, last_gate = combined_all(
        (local_top, local_total, local_sum, last_local), "kv", combine_parts
    )
    top = top + last_gate + forget_log
    own = jnp.sum(
        query_heads.astype(jnp.float32) * new_key.reshape(seqs, heads_here, -1).astype(jnp.float32),
        axis=-1,
    ) * head_size ** (-0.5)
    overall = jnp.maximum(top, own)
    cache_factor = jnp.exp(top - overall)
    own_weight = jnp.exp(own - overall)
    denominator = totals * cache_factor + own_weight
    numerator = summed * cache_factor[..., None] + own_weight[..., None] * new_value.reshape(
        seqs, heads_here, -1
    ).astype(jnp.float32)
    mixed = (numerator / denominator[..., None]).astype(jnp.bfloat16).reshape(seqs, -1)
    partial_value = jnp.dot(mixed, w_out, preferred_element_type=jnp.float32).astype(jnp.bfloat16)
    attended = lax.psum_scatter(partial_value, "tp", scatter_dimension=1, tiled=True).astype(
        jnp.float32
    )
    residual = (tokens.astype(jnp.float32) + attended).astype(jnp.bfloat16)
    mixer = channel_mix(residual, gain_mixer, w_up, w_down, kv_index)
    return (residual.astype(jnp.float32) + mixer).astype(jnp.bfloat16)


f32, bf16 = jnp.float32, jnp.bfloat16
LANES = 128


def spread_rows(rows, width):
    shape = (rows, width)
    return lax.broadcasted_iota(jnp.int32, shape, 0), lax.broadcasted_iota(jnp.int32, shape, 1)


def to_row(column):
    row, lane = spread_rows(column.shape[0], LANES)
    return jnp.sum(jnp.where(row == lane, column, 0.0), axis=0, keepdims=True)


def to_column(line, count):
    row, lane = spread_rows(count, LANES)
    return jnp.sum(jnp.where(row == lane, line, 0.0), axis=-1, keepdims=True)


def fused(
    n_kv,
    n_tp,
    tokens,
    gain_attn_any,
    forget_bias_any,
    lengths_any,
    gain_mixer_any,
    w_query,
    w_key,
    w_value,
    w_forget,
    keys_cache,
    values_cache,
    gates_cache,
    w_out,
    w_up,
    w_down,
    out,
    gain_attn,
    gain_mixer,
    forget_bias,
    lengths,
    wq,
    wk,
    wv,
    wf,
    keys,
    values,
    gates,
    wo,
    wu,
    wd,
    bias,
    logits,
    weights,
    tok_all,
    q_all,
    p_send,
    p_all,
    s_all,
    g_all,
    t_all,
    n_all,
    a_all,
    o_all,
    u_send,
    u_all,
    h_all,
    f_send,
    f_all,
    query,
    coef,
    mid,
    res,
    load_sem,
    kv_out,
    kv_in,
    tp_out,
    tp_in,
    u_out,
    u_in,
    h_out,
    h_in,
):
    kv, tp = lax.axis_index("kv"), lax.axis_index("tp")
    seqs, piece = tok_all.shape[1:]
    rows, cols = wq.shape
    positions = keys.shape[1]
    heads = gates.shape[1]
    all_heads = wf.shape[0]
    size = cols // heads
    mine = seqs // n_kv
    width = gain_attn.shape[0]
    q_parts, q_rows = q_all.shape[1:3]
    a_parts, a_rows = a_all.shape[1:3]
    n_own, chunks = h_all.shape[:2]
    part = h_all.shape[3]
    first = (n_kv - n_own) // 2
    upper = kv // (n_kv // 2)
    is_owner = jnp.logical_and(kv >= first, kv < first + n_own)
    never = -3e38

    barrier = pltpu.get_barrier_semaphore()
    for j in range(1, n_tp):
        pl.semaphore_signal(
            barrier,
            inc=1,
            device_id=(kv, lax.rem(tp + j, n_tp)),
            device_id_type=pl.DeviceIdType.MESH,
        )
    turn = 2 * upper - 1

    def kv_peer(j):
        return lax.rem(kv + turn * j + n_kv, n_kv)

    for j in range(1, n_kv):
        pl.semaphore_signal(
            barrier,
            inc=1,
            device_id=(kv_peer(j), tp),
            device_id_type=pl.DeviceIdType.MESH,
        )

    row_at = pl.multiple_of(kv * rows, rows)
    sources = [
        (tokens, tok_all.at[tp]),
        (lengths_any, lengths),
        (gain_attn_any, gain_attn),
        (forget_bias_any, forget_bias),
        (gain_mixer_any, gain_mixer),
        (gates_cache, gates),
        (w_query, wq),
        (w_forget.at[:, pl.ds(row_at, rows)], wf),
        (w_key, wk),
        (w_value, wv),
        (keys_cache, keys),
        (values_cache, values),
        (w_out, wo),
        (w_up, wu),
        (w_down, wd),
    ]
    loads = [pltpu.make_async_copy(a, b, load_sem.at[i]) for i, (a, b) in enumerate(sources)]
    for load in loads:
        load.start()
    (
        ld_tok,
        ld_len,
        ld_ga,
        ld_bias,
        ld_gm,
        ld_gates,
        ld_q,
        ld_f,
        ld_k,
        ld_v,
        ld_keys,
        ld_values,
        ld_o,
        ld_u,
        ld_d,
    ) = loads

    def remote(source, target, out_sem, in_sem, device):
        return pltpu.make_async_remote_copy(
            src_ref=source,
            dst_ref=target,
            send_sem=out_sem,
            recv_sem=in_sem,
            device_id=device,
            device_id_type=pl.DeviceIdType.MESH,
        )

    pending = []

    def flush():
        for many, sem in pending:
            remote(many, many, sem, sem, (kv_peer(1), tp)).wait_send()
        pending.clear()

    def landed(many, sem):
        remote(many, many, sem, sem, (kv_peer(1), tp)).wait_recv()

    def spread_kv(phase, slot):
        for j in range(1, n_kv):
            remote(
                slot(kv), slot(kv), kv_out.at[phase], kv_in.at[phase], (kv_peer(j), tp)
            ).start()
        pending.append((slot(pl.ds(0, n_kv - 1)), kv_out.at[phase]))

    def gather_kv(phase, slot):
        landed(slot(pl.ds(0, n_kv - 1)), kv_in.at[phase])

    def spread_tp(phase, slot):
        for j in range(1, n_tp):
            remote(
                slot(tp),
                slot(tp),
                tp_out.at[phase],
                tp_in.at[phase],
                (kv, lax.rem(tp + j, n_tp)),
            ).start()
        pending.append((slot(pl.ds(0, n_tp - 1)), tp_out.at[phase]))

    def gather_tp(phase, slot):
        landed(slot(pl.ds(0, n_tp - 1)), tp_in.at[phase])

    def total_of(read):
        total = read(0).astype(f32)
        for o in range(1, n_kv):
            total = total + read(o).astype(f32)
        return total

    ld_tok.wait()
    pl.semaphore_wait(barrier, n_kv + n_tp - 2)
    spread_tp(0, lambda t: tok_all.at[t])

    ld_len.wait()
    ld_ga.wait()
    ld_bias.wait()
    ld_gm.wait()
    ld_gates.wait()
    lane_seq = lax.broadcasted_iota(jnp.int32, (1, LANES), 1) // heads
    place = kv * positions + lax.broadcasted_iota(jnp.int32, (heads, positions), 1)
    lasts = []
    for b in range(seqs):
        gate = gates[b]
        length = lengths[b]
        bias[b * heads : (b + 1) * heads] = jnp.where(place < length, -gate, never)
        last = jnp.where(place == length - 1, gate, 0.0)
        lasts.append(jnp.sum(last, axis=-1, keepdims=True))
    last_row = to_row(jnp.concatenate(lasts, axis=0))
    gain_a = gain_attn[pl.ds(row_at, rows)].astype(f32).reshape(1, rows)
    gain_m = gain_mixer[pl.ds(row_at, rows)].astype(f32).reshape(1, rows)

    gather_tp(0, lambda t: tok_all.at[t])
    tok = jnp.concatenate([tok_all[t] for t in range(n_tp)], axis=1).astype(f32)
    scaled = (tok * gain_a).astype(bf16)
    ld_q.wait()
    q_part = jnp.dot(scaled, wq[...], preferred_element_type=f32).astype(bf16)
    s_all[0, kv] = to_row(jnp.sum(tok * tok, axis=-1, keepdims=True))
    for c in range(q_parts):
        q_all[kv, c] = q_part[c * q_rows : (c + 1) * q_rows]
    spread_kv(0, lambda o: s_all.at[0, o])
    for c in range(q_parts):
        spread_kv(1 + c, lambda o, c=c: q_all.at[o, c])

    ld_k.wait()
    ld_v.wait()
    ld_f.wait()
    part_key = jnp.dot(scaled, wk[...], preferred_element_type=f32)
    part_value = jnp.dot(scaled, wv[...], preferred_element_type=f32)
    for o in range(n_kv):
        at = slice(o * mine, (o + 1) * mine)
        p_send[o, :, :cols] = part_key[at]
        p_send[o, :, cols:] = part_value[at]
    for j in range(1, n_kv):
        peer = kv_peer(j)
        remote(
            p_send.at[peer], p_all.at[kv], kv_out.at[P_PHASE], kv_in.at[P_PHASE], (peer, tp)
        ).start()
    pending.append((p_send.at[pl.ds(0, n_kv - 1)], kv_out.at[P_PHASE]))
    p_all[kv] = p_send[kv]

    part_gate = lax.dot_general(
        scaled, wf[...], (((1,), (1,)), ((), ())), preferred_element_type=f32
    )
    tall = jnp.concatenate(
        [part_gate, jnp.broadcast_to(forget_bias[...], (8, all_heads))], axis=0
    )
    head_lane = lax.broadcasted_iota(jnp.int32, tall.shape, 1) - tp * heads
    lane_head = lax.broadcasted_iota(jnp.int32, (1, LANES), 1) % heads
    wide = jnp.zeros((seqs + 8, LANES), f32)
    for h in range(heads):
        column = jnp.sum(jnp.where(head_lane == h, tall, 0.0), axis=-1, keepdims=True)
        wide = jnp.where(lane_head == h, column, wide)
    seq_row = lax.broadcasted_iota(jnp.int32, (seqs, LANES), 0)
    here = seq_row == lane_seq
    g_all[kv, 0:1, :] = jnp.sum(jnp.where(here, wide[:seqs], 0.0), axis=0, keepdims=True)
    g_all[kv, 1:2, :] = last_row
    spread_kv(G_PHASE, lambda o: g_all.at[o])
    bias_row = wide[seqs : seqs + 1]

    gather_kv(0, lambda o: s_all.at[0, o])
    squares = to_column(total_of(lambda o: s_all[0, o]), seqs)
    attn_scale = lax.rsqrt(squares / width + norm_eps)
    query[:, cols:] = jnp.broadcast_to(attn_scale, (seqs, LANES))
    own_block = (
        lax.broadcasted_iota(jnp.int32, (heads, cols), 0)
        == lax.broadcasted_iota(jnp.int32, (heads, cols), 1) // size
    )
    ld_keys.wait()
    for c in range(q_parts):
        gather_kv(1 + c, lambda o, c=c: q_all.at[o, c])
        q_here = total_of(lambda o, c=c: q_all[o, c])
        q_here = (attn_scale[c * q_rows : (c + 1) * q_rows] * q_here).astype(bf16).astype(f32)
        query[c * q_rows : (c + 1) * q_rows, :cols] = q_here
        for r in range(0, q_rows, 2):
            pair = [jnp.where(own_block, q_here[r + i : r + i + 1], 0.0) for i in range(2)]
            pair = jnp.concatenate(pair, axis=0).astype(bf16)
            for i in range(2):
                b = c * q_rows + r + i
                scores = lax.dot_general(
                    pair, keys[b], (((1,), (1,)), ((), ())), preferred_element_type=f32
                )
                logits[b * heads : (b + 1) * heads] = scores[i * heads : (i + 1) * heads]

    scores = logits[...] * size ** (-0.5) + bias[...]
    top = jnp.maximum(jnp.max(scores, axis=-1, keepdims=True), -1e30)
    spread = jnp.exp(scores - top)
    weights[...] = spread.astype(bf16)
    t_all[kv, 0:1, :] = to_row(top)
    t_all[kv, 1:2, :] = to_row(jnp.sum(spread, axis=-1, keepdims=True))
    spread_kv(T_PHASE, lambda o: t_all.at[o])
    ld_values.wait()

    def attend(pair):
        left = weights[pair * 2 * heads : (pair + 1) * 2 * heads]
        found = []
        for r in range(2):
            summed = jnp.dot(left, values[2 * pair + r], preferred_element_type=f32)
            summed = jnp.where(own_block, summed[r * heads : (r + 1) * heads], 0.0)
            found.append(jnp.sum(summed, axis=0, keepdims=True))
        return found

    def own_token():
        gather_kv(P_PHASE, lambda o: p_all.at[o])
        gather_kv(G_PHASE, lambda o: g_all.at[o])
        scale_row = jnp.sum(jnp.where(here, attn_scale, 0.0), axis=0, keepdims=True)
        gate_sum = total_of(lambda o: g_all[o])
        gate_logit = scale_row * gate_sum[0:1] + bias_row
        forget_log = jnp.minimum(gate_logit, 0.0) - jnp.log1p(jnp.exp(-jnp.abs(gate_logit)))
        p_total = total_of(lambda o: p_all[o])
        own_rows = [query[pl.ds(kv * mine + r, 1), :] for r in range(mine)]
        own_query = jnp.concatenate(own_rows, axis=0)
        own_scale = own_query[:, cols : cols + 1]
        new_key = (own_scale * p_total[:, :cols]).astype(bf16).astype(f32)
        n_all[kv, :, :cols] = (own_scale * p_total[:, cols:]).astype(bf16).astype(f32)
        product = own_query[:, :cols] * new_key
        col_head = lax.broadcasted_iota(jnp.int32, (mine, cols), 1) // size
        own = jnp.full((mine, LANES), never, f32)
        own_seq = kv * mine + lax.broadcasted_iota(jnp.int32, (mine, LANES), 0)
        for h in range(heads):
            column = jnp.sum(jnp.where(col_head == h, product, 0.0), axis=-1, keepdims=True)
            at = jnp.logical_and(lane_head == h, lane_seq == own_seq)
            own = jnp.where(at, column * size ** (-0.5), own)
        own = own - jnp.where(lane_seq == own_seq, gate_sum[1:2] + forget_log, 0.0)
        n_all[kv, :, cols:] = own
        spread_kv(N_PHASE, lambda o: n_all.at[o])

    def weigh_parts():
        gather_kv(T_PHASE, lambda o: t_all.at[o])
        gather_kv(N_PHASE, lambda o: n_all.at[o])
        own = jnp.max(n_all[0, :, cols:], axis=0, keepdims=True)
        for o in range(1, n_kv):
            own = jnp.maximum(own, jnp.max(n_all[o, :, cols:], axis=0, keepdims=True))
        tops = [t_all[o, 0:1, :] for o in range(n_kv)] + [own]
        totals = [t_all[o, 1:2, :] for o in range(n_kv)] + [jnp.ones((1, LANES), f32)]
        overall = functools.reduce(jnp.maximum, tops)
        factors = [jnp.exp(one - overall) for one in tops]
        denominator = sum(one * total for one, total in zip(factors, totals))
        stack = jnp.concatenate(
            [jnp.where(here, one / denominator, 0.0) for one in factors], axis=0
        )
        high = stack.astype(bf16)
        low = (stack - high.astype(f32)).astype(bf16)
        lane = lax.broadcasted_iota(jnp.int32, (2 * LANES, cols), 0) % heads
        same = lane == lax.broadcasted_iota(jnp.int32, (2 * LANES, cols), 1) // size
        coef[...] = jnp.dot(
            jnp.concatenate([high, low], axis=1),
            jnp.where(same, 1.0, 0.0).astype(bf16),
            preferred_element_type=f32,
        )

    own_token()
    pairs_per = a_rows // 2
    for c in range(a_parts):
        found = []
        for i in range(pairs_per):
            found.extend(attend(c * pairs_per + i))
        a_all[kv, c] = jnp.concatenate(found, axis=0).astype(bf16)
        spread_kv(A_PHASE + c, lambda o, c=c: a_all.at[o, c])
    flush()
    weigh_parts()
    ld_o.wait()
    added = []
    new_values = jnp.concatenate([n_all[o, :, :cols] for o in range(n_kv)], axis=0)
    for c in range(a_parts):
        gather_kv(A_PHASE + c, lambda o, c=c: a_all.at[o, c])
        own_at = n_kv * seqs + c * a_rows
        mixed = coef[own_at : own_at + a_rows] * new_values[c * a_rows : (c + 1) * a_rows]
        for o in range(n_kv):
            at = o * seqs + c * a_rows
            mixed = mixed + coef[at : at + a_rows] * a_all[o, c].astype(f32)
        added.append(mixed)
    mixed = jnp.concatenate(added, axis=0).astype(bf16)
    o_all[tp] = jnp.dot(mixed, wo[...], preferred_element_type=f32).astype(bf16)
    spread_tp(1, lambda t: o_all.at[t])
    ld_u.wait()
    flush()
    gather_tp(1, lambda t: o_all.at[t])
    attended = o_all[0].astype(f32)
    for t in range(1, n_tp):
        attended = attended + o_all[t].astype(f32)
    residual = (tok + attended).astype(bf16).astype(f32)
    for t in range(n_tp):
        res[t] = residual[:, t * piece : (t + 1) * piece]
    mid[...] = (residual * gain_m).astype(bf16)
    s_all[1, kv] = to_row(jnp.sum(residual * residual, axis=-1, keepdims=True))
    own_m = kv - first

    def mixer_part(owner):
        if not owner:
            order = [(n_own // 2 + j) % n_own for j in range(n_own)]
            targets = [near + upper * (n_own - 1 - 2 * near) for near in order]
        elif n_own == n_kv:
            targets = [kv_peer(j) for j in range(1, n_kv)]
        else:
            order = [n_own // 2, *range(n_own // 2 + 1, n_own), *range(1, n_own // 2)]
            targets = [lax.rem(own_m + j, n_own) for j in order]
        count = len(targets)
        for m in targets:
            remote(
                s_all.at[1, kv],
                s_all.at[1, kv],
                u_out.at[chunks],
                u_in.at[chunks],
                (first + m, tp),
            ).start()

        def up_piece(m, c):
            at = pl.multiple_of((m * chunks + c) * part, part)
            u_send[c, m] = jnp.dot(
                mid[...], wu[:, pl.ds(at, part)], preferred_element_type=f32
            ).astype(bf16)

        for c in range(chunks):
            for m in targets:
                up_piece(m, c)
            for m in targets:
                remote(
                    u_send.at[c, m], u_all.at[c, kv], u_out.at[c], u_in.at[c], (first + m, tp)
                ).start()
        own_order = []
        if owner:
            for c in range(chunks):
                up_piece(own_m, c)
            landed(s_all.at[1, pl.ds(0, n_kv - 1)], u_in.at[chunks])
            squares = to_column(total_of(lambda o: s_all[1, o]), seqs)
            mixer_scale = lax.rsqrt(squares / width + norm_eps)
            for c in range(chunks):
                u_all[c, kv] = u_send[c, own_m]
                landed(u_all.at[c, pl.ds(0, n_kv - 1)], u_in.at[c])
                active = jnp.maximum(mixer_scale * total_of(lambda o, c=c: u_all[c, o]), 0.0)
                h_all[own_m, c] = (active * active).astype(bf16)
                for j in range(1, n_kv):
                    remote(
                        h_all.at[own_m, c],
                        h_all.at[own_m, c],
                        h_out.at[c],
                        h_in.at[c, own_m],
                        (kv_peer(j), tp),
                    ).start()
                own_order.append((c, own_m))

        def down_piece(m, c):
            at = pl.multiple_of((m * chunks + c) * part, part)
            return jnp.dot(h_all[m, c], wd[pl.ds(at, part), :], preferred_element_type=f32)

        ld_d.wait()
        for c in range(chunks):
            many = u_send.at[c, pl.ds(0, count)]
            remote(many, many, u_out.at[c], u_out.at[c], (kv_peer(1), tp)).wait_send()
        many = s_all.at[1, pl.ds(0, count)]
        remote(many, many, u_out.at[chunks], u_out.at[chunks], (kv_peer(1), tp)).wait_send()
        down = jnp.zeros((seqs, rows), f32)
        for c, m in own_order:
            down = down + down_piece(m, c)
        for c in range(chunks):
            for m in reversed(targets):
                landed(h_all.at[m, c], h_in.at[c, m])
                down = down + down_piece(m, c)
        for t in range(n_tp):
            f_send[t] = down[:, t * piece : (t + 1) * piece].astype(bf16)
        for j in range(1, n_tp):
            peer = lax.rem(tp + j, n_tp)
            remote(
                f_send.at[peer], f_all.at[tp], tp_out.at[2], tp_in.at[2], (kv, peer)
            ).start()
        f_all[tp] = f_send[tp]
        if owner:
            for c in range(chunks):
                many = u_all.at[c, pl.ds(0, n_kv - 1)]
                remote(many, many, h_out.at[c], h_out.at[c], (kv_peer(1), tp)).wait_send()

    if n_own == n_kv:
        mixer_part(True)
    else:
        pl.when(is_owner)(lambda: mixer_part(True))
        pl.when(jnp.logical_not(is_owner))(lambda: mixer_part(False))
    pending.append((f_send.at[pl.ds(0, n_tp - 1)], tp_out.at[2]))
    flush()
    gather_tp(2, lambda t: f_all.at[t])
    mixer = f_all[0].astype(f32)
    for t in range(1, n_tp):
        mixer = mixer + f_all[t].astype(f32)
    out[...] = (res[tp] + mixer).astype(bf16)


Q_PARTS = 2
A_PARTS = 2
CHUNKS = 2
OWNERS = 2
P_PHASE = 1 + Q_PARTS
G_PHASE = P_PHASE + 1
T_PHASE = G_PHASE + 1
N_PHASE = T_PHASE + 1
A_PHASE = N_PHASE + 1
PHASES = A_PHASE + A_PARTS


def layer(n_kv, n_tp, *arrays):
    (
        tokens,
        gain_attn,
        w_query,
        w_key,
        w_value,
        w_forget,
        forget_bias,
        keys_cache,
        values_cache,
        gates_cache,
        lengths,
        w_out,
        gain_mixer,
        w_up,
        w_down,
    ) = arrays
    seqs, piece = tokens.shape
    rows, cols = w_query.shape
    positions = keys_cache.shape[1]
    heads = gates_cache.shape[1]
    all_heads = w_forget.shape[1]
    n_own = n_kv // OWNERS
    part = w_up.shape[1] // max(n_own * CHUNKS, 1)
    fits = (
        n_kv % 4 == 0
        and n_tp > 1
        and seqs % n_kv == 0
        and seqs * heads == LANES
        and heads % 8 == 0
        and seqs % (8 * max(Q_PARTS, A_PARTS)) == 0
        and piece % LANES == 0
        and cols % LANES == 0
        and positions % LANES == 0
        and part % LANES == 0
        and w_up.shape[1] == part * n_own * CHUNKS
        and all_heads <= LANES
        and w_out.shape == (cols, rows)
        and rows == n_tp * piece
    )
    if not fits:
        return shards(*arrays)
    mine = seqs // n_kv
    vmem = pl.BlockSpec(memory_space=pltpu.VMEM)
    anywhere = pl.BlockSpec(memory_space=pl.ANY)
    bias = forget_bias.reshape(1, -1)

    def like(x):
        return pltpu.VMEM(x.shape, x.dtype)

    return pl.pallas_call(
        functools.partial(fused, n_kv, n_tp),
        out_shape=jax.ShapeDtypeStruct((seqs, piece), bf16),
        in_specs=[anywhere] * 15,
        out_specs=vmem,
        scratch_shapes=[
            like(gain_attn),
            like(gain_mixer),
            like(bias),
            pltpu.SMEM(lengths.shape, lengths.dtype),
            like(w_query),
            like(w_key),
            like(w_value),
            pltpu.VMEM((all_heads, rows), bf16),
            like(keys_cache),
            like(values_cache),
            like(gates_cache),
            like(w_out),
            like(w_up),
            like(w_down),
            pltpu.VMEM((seqs * heads, positions), f32),
            pltpu.VMEM((seqs * heads, positions), f32),
            pltpu.VMEM((seqs * heads, positions), bf16),
            pltpu.VMEM((n_tp, seqs, piece), bf16),
            pltpu.VMEM((n_kv, Q_PARTS, seqs // Q_PARTS, cols), bf16),
            pltpu.VMEM((n_kv, mine, 2 * cols), f32),
            pltpu.VMEM((n_kv, mine, 2 * cols), f32),
            pltpu.VMEM((2, n_kv, 1, LANES), f32),
            pltpu.VMEM((n_kv, 2, LANES), f32),
            pltpu.VMEM((n_kv, 2, LANES), f32),
            pltpu.VMEM((n_kv, mine, cols + LANES), f32),
            pltpu.VMEM((n_kv, A_PARTS, seqs // A_PARTS, cols), bf16),
            pltpu.VMEM((n_tp, seqs, rows), bf16),
            pltpu.VMEM((CHUNKS, n_own, seqs, part), bf16),
            pltpu.VMEM((CHUNKS, n_kv, seqs, part), bf16),
            pltpu.VMEM((n_own, CHUNKS, seqs, part), bf16),
            pltpu.VMEM((n_tp, seqs, piece), bf16),
            pltpu.VMEM((n_tp, seqs, piece), bf16),
            pltpu.VMEM((seqs, cols + LANES), f32),
            pltpu.VMEM(((n_kv + 1) * seqs, cols), f32),
            pltpu.VMEM((seqs, rows), bf16),
            pltpu.VMEM((n_tp, seqs, piece), f32),
            pltpu.SemaphoreType.DMA((15,)),
            pltpu.SemaphoreType.DMA((PHASES,)),
            pltpu.SemaphoreType.DMA((PHASES,)),
            pltpu.SemaphoreType.DMA((3,)),
            pltpu.SemaphoreType.DMA((3,)),
            pltpu.SemaphoreType.DMA((CHUNKS + 1,)),
            pltpu.SemaphoreType.DMA((CHUNKS + 1,)),
            pltpu.SemaphoreType.DMA((CHUNKS,)),
            pltpu.SemaphoreType.DMA((CHUNKS, n_own)),
        ],
        compiler_params=pltpu.CompilerParams(
            collective_id=0, has_side_effects=True, vmem_limit_bytes=VMEM_LIMIT
        ),
    )(
        tokens,
        gain_attn,
        bias,
        lengths,
        gain_mixer,
        w_query,
        w_key,
        w_value,
        w_forget.T,
        keys_cache,
        values_cache,
        gates_cache,
        w_out,
        w_up,
        w_down,
    )


VMEM_LIMIT = 60 * 1024 * 1024


def solution(mesh):
    return jax.shard_map(
        functools.partial(layer, mesh.shape["kv"], mesh.shape["tp"]),
        mesh=mesh,
        in_specs=(
            P(None, ("kv", "tp")),
            P(),
            P("kv", "tp"),
            P("kv", "tp"),
            P("kv", "tp"),
            P(),
            P(),
            P(None, "kv", "tp"),
            P(None, "kv", "tp"),
            P(None, "tp", "kv"),
            P(),
            P("tp", "kv"),
            P(),
            P("kv", "tp"),
            P("tp", "kv"),
        ),
        out_specs=P(None, ("kv", "tp")),
        check_vma=False,
    )
```
